256 devices in a mesh: grp: 2 (over y), ep: 32 (over z, core), tp: 4 (over x).
Axes of the slice: x: 4, y: 2, z: 16, core: 2. Of those that a mesh axis runs over, the one named last changes fastest.
The devices are a block of a 4x16x16 slice.
Arguments:
- query_rows: bfloat16 [12288, 2048], P(('grp', 'ep'), 'tp'), parts along dimension 0, may hold values from -100 to 100
- projected_keys: bfloat16 [12288, 512], P(('grp', 'ep'), 'tp'), parts along dimension 0, may hold values from -100 to 100
- projected_values: bfloat16 [12288, 512], P(('grp', 'ep'), 'tp'), parts along dimension 0, may hold values from -6 to 6
- query_gain: float32 [128], replicated, may hold values from 0.3 to 6.5
- key_norm_gain: float32 [128], replicated, may hold values from 0.3 to 6.5
- out_proj: bfloat16 [2048, 2048], P('tp'), may hold values from -4 to 4
- mix_tokens: bfloat16 [32768, 2048], P(('grp', 'ep', 'tp')), parts along dimension 0, may hold values from -150 to 150
- norm_gain: float32 [2048], replicated, may hold values from 0.1 to 1.9
- expert_ids: int32 [32768, 2], P(('grp', 'ep', 'tp')), parts along dimension 0, may hold values from 0 to 31, all different within a row; in each aligned block of 128 rows (0 to 127, 128 to 255, ...) at most 12 rows name the same one
- expert_score: float32 [32768, 2], P(('grp', 'ep', 'tp')), parts along dimension 0, may hold values from -6 to 6
- gate_proj: bfloat16 [32, 2048, 2048], P('ep', None, 'tp'), may hold values from -0.125 to 0.125
- up_proj: bfloat16 [32, 2048, 2048], P('ep', None, 'tp'), may hold values from -0.125 to 0.125
- down_proj: bfloat16 [32, 2048, 2048], P('ep', 'tp'), may hold values from -0.125 to 0.125
Outputs:
- mixed_rows: bfloat16 [12288, 2048], P(('grp', 'ep', 'tp')), parts along dimension 0
- expert_out: bfloat16 [32768, 2048], P(('grp', 'ep', 'tp')), parts along dimension 0
The draws below stay inside these ranges and needn't reach their ends.
There are 2 independent parts, one for each index of `grp`. The reference program is written for one: setup_inputs(seed, part) draws one part's arguments, and reference() takes and returns one part's arrays. A program takes and returns all parts, laid end to end along the dimension named above; an argument that names none is the same for every part. Nothing has to cross between parts.
Inputs may be any that keep to these rules, and one draw needn't show every extreme that they name: `expert_ids`: each row names 2 different experts. Within the rows of one device (aligned blocks of 128 rows) no expert is named more than 12 times, and in every draw some device names some expert exactly 12 times.
All inputs are finite; a program needn't handle non-finite values.
Results may differ from the reference program's by a relative error of at most 0.014.
The reference program's roundings to bfloat16 on the way count: a program that leaves them out, or rounds other values in their place, can miss the bound.
Values may be sent and summed in bfloat16 or wider, within the bound.
No kernel may reach another device: no remote copies, remote signals or barrier semaphores. Data moves between devices by JAX's collectives and lax.ppermute only.
A program may use at most 128 MiB of HBM per device.

```python
import math
import jax
import jax.numpy as jnp
import numpy as np
from jax import lax

D = 2048
HEAD_SIZE = 128
QUERY_HEADS = 16
KEY_VALUE_HEADS = 4
GRID_W = 64
FFE = 2048
TOPK = 2
TOK_B_DEV = 128
EXPERTS = 32
ATTENTION_TOKENS = 6144
TOKENS_B = 16384
CAP = 12
N_TP = 4


def attention_pair(key):
    folded = jax.random.fold_in(key, 11)
    keys_by_head = jax.random.split(folded, 4)
    query_matrix = jnp.clip(jax.random.normal(keys_by_head[0], (ATTENTION_TOKENS, QUERY_HEADS, HEAD_SIZE), jnp.float32), -5.0, 5.0)
    query_matrix = query_matrix * jnp.exp(jax.random.uniform(keys_by_head[1], (ATTENTION_TOKENS, QUERY_HEADS, 1), jnp.float32) * math.log(10.0))
    key_value_pairs = jnp.clip(jax.random.normal(keys_by_head[2], (ATTENTION_TOKENS, KEY_VALUE_HEADS, HEAD_SIZE), jnp.float32), -5.0, 5.0)
    key_value_pairs = key_value_pairs * jnp.exp(jax.random.uniform(keys_by_head[3], (ATTENTION_TOKENS, KEY_VALUE_HEADS, 1), jnp.float32) * math.log(10.0))
    query_matrix = jnp.clip(query_matrix, -100.0, 100.0).reshape(ATTENTION_TOKENS, QUERY_HEADS * HEAD_SIZE)
    key_value_pairs = jnp.clip(key_value_pairs, -100.0, 100.0).reshape(ATTENTION_TOKENS, KEY_VALUE_HEADS * HEAD_SIZE)
    return (query_matrix, key_value_pairs)


def draw_query_rows(key, part):
    return attention_pair(key)[0].astype(jnp.bfloat16)


def draw_projected_keys(key, part):
    return attention_pair(key)[1].astype(jnp.bfloat16)


def gain_draw(key):
    return jnp.clip(1.0 + 0.18 * jax.random.normal(key, (HEAD_SIZE,), jnp.float32), 0.3, 1.9)


def draw_query_gain(key, part):
    return gain_draw(jax.random.fold_in(key, 21))


def draw_key_norm_gain(key, part):
    return gain_draw(jax.random.fold_in(key, 22))


def draw_mix_tokens(key, part):
    keys_by_head = jax.random.split(jax.random.fold_in(key, 31), 3)
    row_scale = jnp.exp(jax.random.uniform(keys_by_head[1], (TOKENS_B, 1), jnp.float32) * math.log(10.0))
    col_scale = jnp.exp(jax.random.uniform(keys_by_head[2], (1, D), jnp.float32, math.log(0.3), math.log(3.0)))
    entries = jnp.clip(jax.random.normal(keys_by_head[0], (TOKENS_B, D), jnp.float32), -5.0, 5.0)
    return jnp.clip(entries * row_scale * col_scale, -150.0, 150.0).astype(jnp.bfloat16)


def level_of(stream_key, shape, shards, low, largest):
    level, own = 1.0, jax.random.fold_in(stream_key, 6)
    for axis_at, parts in shards:
        draws = jnp.exp(jax.random.uniform(jax.random.fold_in(own, axis_at), (parts,), jnp.float32, low / len(shards), largest / len(shards)))
        level = level * jnp.repeat(draws, shape[axis_at] // parts).reshape([-1 if axis == axis_at else 1 for axis in range(len(shape))])
    return level


def routed_block(stream_key, own, number, rows, count, top, most, lean):
    order = jax.random.permutation(stream_key, count)
    packed, usual = shares(count, rows * top, most, lean, True), shares(count, rows * top, most, lean, False)
    places = jnp.arange(count)

    def named(sizes, rotation):
        used = int((sizes > 0).sum())
        fixed = max(1, used // 4)
        moved = fixed + (places - fixed + rotation * (used - fixed)) % max(1, count - fixed)
        return jnp.zeros((count,), jnp.int32).at[order[jnp.where(places < fixed, places, moved)]].set(jnp.asarray(sizes, jnp.int32))

    sizes = jnp.where(number % 4 == 0, named(packed, number // 4), named(usual, number - number // 4 - 1))
    mixed = jax.random.permutation(jax.random.fold_in(own, 3), count)
    source_of, sink = mixed[0:count // 2 * 2:2], mixed[1:count // 2 * 2:2]
    room = jnp.minimum(sizes[source_of] - 1, most - sizes[sink]) // 2
    room = jnp.where((source_of == order[0]) | (sink == order[0]) | (sizes[sink] == 0), 0, jnp.maximum(room, 0))
    moved = jax.random.randint(jax.random.fold_in(own, 4), (count // 2,), 0, 1 << 20) % (room + 1)
    sizes = sizes.at[source_of].add(-moved).at[sink].add(moved)
    labels = jnp.searchsorted(jnp.cumsum(sizes), jnp.arange(rows * top), side="right").astype(jnp.int32)
    listing = labels.reshape(top, rows).T
    listing = listing[jax.random.permutation(jax.random.fold_in(own, 1), rows)]
    rotation = jax.random.randint(jax.random.fold_in(own, 2), (rows, 1), 0, top)
    return jnp.take_along_axis(listing, (jnp.arange(top)[None, :] + rotation) % top, axis=1)


def shares(amount, total, reach, slope, full):
    loads = [(1 << 20) // math.isqrt(rank ** slope) + 1 for rank in range(1, amount + 1)]
    largest = reach if full else min(reach, max(-(-total // amount), total * loads[0] // sum(loads)))
    least = 1 if total - largest >= amount - 1 else 0
    given, rest = [largest] + [least] * (amount - 1), total - largest - least * (amount - 1)
    while rest > 0:
        candidates = [i for i in range(1, amount) if given[i] < largest] or [i for i in range(1, amount) if given[i] < reach]
        pool, remaining = sum([loads[i] for i in candidates]), rest
        for i in candidates:
            extra = min(reach - given[i], max(1, remaining * loads[i] // pool), rest)
            given[i] = given[i] + extra
            rest = rest - extra
    return np.array(given)


def gaussian(stream_key, dims, deviation, bound, cuts=(), kind=jnp.bfloat16):
    result = deviation * jax.random.normal(stream_key, dims, jnp.float32)
    if cuts:
        result = result * level_of(stream_key, dims, cuts, -0.22, 0.18)
    return jnp.clip(result, -bound, bound).astype(kind)


def setup_inputs(seed: int = 0, part: int = 0) -> dict:
    keys = jax.random.split(jax.random.key(seed), 14)
    part_splits = jax.random.split(jax.random.fold_in(keys[13], part), 14)
    query_rows = draw_query_rows(jax.random.fold_in(jax.random.fold_in(keys[13], part), 71), part)
    projected_keys = draw_projected_keys(jax.random.fold_in(jax.random.fold_in(keys[13], part), 71), part)
    projected_values = gaussian(part_splits[2], (ATTENTION_TOKENS, KEY_VALUE_HEADS * HEAD_SIZE), 1.0, 6.0, ((0, 32), (1, 4)))
    query_gain = draw_query_gain(jax.random.fold_in(keys[13], 71), part)
    key_norm_gain = draw_key_norm_gain(jax.random.fold_in(keys[13], 71), part)
    out_proj = gaussian(keys[5], (QUERY_HEADS * HEAD_SIZE, D), (max(1, QUERY_HEADS * HEAD_SIZE // 1024)) ** -0.5, 4.0, ((0, 4),))
    mix_tokens = draw_mix_tokens(jax.random.fold_in(jax.random.fold_in(keys[13], part), 71), part)
    norm_gain = jnp.clip(1.0 + 0.18 * jax.random.normal(keys[7], (D,), jnp.float32), 0.1, 1.9)
    expert_ids_keys = jax.random.split(jax.random.fold_in(part_splits[8], 1), TOKENS_B // TOK_B_DEV)
    expert_ids_turns = jax.random.permutation(jax.random.fold_in(part_splits[8], 3), TOKENS_B // TOK_B_DEV)
    expert_ids = jax.vmap(lambda own, number: routed_block(jax.random.fold_in(part_splits[8], 2), own, number, TOK_B_DEV, EXPERTS, TOPK, CAP, 2))(expert_ids_keys, expert_ids_turns).reshape((TOKENS_B, TOPK))
    expert_score = gaussian(part_splits[9], (TOKENS_B, TOPK), 1.5, 6.0, ((0, 128),), jnp.float32)
    gate_proj = gaussian(keys[10], (EXPERTS, D, FFE), D ** -0.5, 0.125, ((0, 32), (2, 4)))
    up_proj = gaussian(keys[11], (EXPERTS, D, FFE), D ** -0.5, 0.125, ((0, 32), (2, 4)))
    down_proj = gaussian(keys[12], (EXPERTS, FFE, D), FFE ** -0.5, 0.125, ((0, 32), (1, 4)))
    return {"query_rows": query_rows, "projected_keys": projected_keys, "projected_values": projected_values, "query_gain": query_gain, "key_norm_gain": key_norm_gain, "out_proj": out_proj, "mix_tokens": mix_tokens, "norm_gain": norm_gain, "expert_ids": expert_ids, "expert_score": expert_score, "gate_proj": gate_proj, "up_proj": up_proj, "down_proj": down_proj}


EPS = 1e-06
THETA = 10000.0

def head_norm(vectors, gain):
    return vectors * lax.rsqrt(lax.optimization_barrier(jnp.mean(vectors * vectors, axis=-1, keepdims=True)) + EPS) * gain

def rotate_grid(vectors, token_positions):
    length, heads, head_dim = vectors.shape
    quarter = head_dim // 4
    freqs = 1.0 / THETA ** (jnp.arange(quarter, dtype=jnp.float32) * 4.0 / head_dim)
    grid_row = (token_positions // GRID_W).astype(jnp.float32)
    grid_col = (token_positions % GRID_W).astype(jnp.float32)
    angles = jnp.stack([grid_row[:, None] * freqs, grid_col[:, None] * freqs], axis=1)
    cosine = jnp.cos(angles)[:, None]
    sine = jnp.sin(angles)[:, None]
    halves = vectors.reshape(length, heads, 2, 2, quarter)
    first = halves[..., 0, :]
    second = halves[..., 1, :]
    turned = jnp.stack([first * cosine - second * sine, second * cosine + first * sine], axis=-2)
    return turned.reshape(length, heads, head_dim)

def prepare_inputs(raw_rows, gain, heads, token_positions):
    length = raw_rows.shape[0]
    vectors = raw_rows.astype(jnp.float32).reshape(length, heads, HEAD_SIZE)
    return rotate_grid(head_norm(vectors, gain), token_positions).astype(jnp.bfloat16)

def reference(query_rows, projected_keys, projected_values, query_gain, key_norm_gain, out_proj, mix_tokens, norm_gain, expert_ids, expert_score, gate_proj, up_proj, down_proj):
    token_total = query_rows.shape[0]
    token_positions = jnp.arange(token_total, dtype=jnp.int32)
    queries_per_group = QUERY_HEADS // KEY_VALUE_HEADS
    query_matrix = prepare_inputs(query_rows, query_gain, QUERY_HEADS, token_positions)
    keys_expanded = prepare_inputs(projected_keys, key_norm_gain, KEY_VALUE_HEADS, token_positions).astype(jnp.float32)
    values_expanded = projected_values.reshape(token_total, KEY_VALUE_HEADS, HEAD_SIZE).astype(jnp.float32)
    rows_per_block = math.gcd(token_total, 256)
    blocked_queries = query_matrix.reshape(token_total // rows_per_block, rows_per_block, KEY_VALUE_HEADS, queries_per_group, HEAD_SIZE)

    def attend(query_block):
        scores = jnp.einsum('tkgd,skd->kgts', query_block.astype(jnp.float32), keys_expanded) * HEAD_SIZE ** (-0.5)
        top_score = lax.optimization_barrier(jnp.max(scores, axis=-1, keepdims=True))
        probs = jnp.exp(scores - top_score)
        prob_total = lax.optimization_barrier(jnp.sum(probs, axis=-1))
        rounded = lax.optimization_barrier(probs.astype(jnp.bfloat16)).astype(jnp.float32)
        summed = jnp.einsum('kgts,skd->tkgd', rounded, values_expanded)
        return (summed / jnp.transpose(prob_total, (2, 0, 1))[..., None]).astype(jnp.bfloat16)
    heads_out = lax.map(attend, blocked_queries).reshape(token_total, QUERY_HEADS * HEAD_SIZE)
    group_width = QUERY_HEADS * HEAD_SIZE // N_TP
    mixed = jnp.zeros((token_total, D), jnp.float32)
    for group_index in range(N_TP):
        lower = group_index * group_width
        partial_value = jnp.dot(heads_out[:, lower:lower + group_width], out_proj[lower:lower + group_width], preferred_element_type=jnp.float32)
        mixed = mixed + lax.optimization_barrier(partial_value.astype(jnp.bfloat16)).astype(jnp.float32)
    mixed_rows = mixed.astype(jnp.bfloat16)
    count_b = mix_tokens.shape[0]
    blocks = count_b // TOK_B_DEV
    values_b = mix_tokens.astype(jnp.float32)
    normed = (values_b * lax.rsqrt(lax.optimization_barrier(jnp.mean(values_b * values_b, axis=-1, keepdims=True)) + EPS) * norm_gain).astype(jnp.bfloat16)
    flat = expert_ids.reshape(blocks, TOK_B_DEV * TOPK)
    onehot = (flat[..., None] == jnp.arange(EXPERTS, dtype=jnp.int32)).astype(jnp.int32)
    slots = lax.optimization_barrier(jnp.sum((jnp.cumsum(onehot, axis=1) - onehot) * onehot, axis=-1))
    owners = jnp.arange(blocks, dtype=jnp.int32)[:, None]
    places = ((flat * blocks + owners) * CAP + slots).reshape(count_b, TOPK).astype(jnp.int32)
    buffer = jnp.zeros((EXPERTS * blocks * CAP, D), jnp.bfloat16)
    for route_slot in range(TOPK):
        buffer = buffer.at[places[:, route_slot]].set(normed)
    stacked = buffer.reshape(EXPERTS, blocks * CAP, D)
    hidden_width = FFE // N_TP

    def run_expert(operands):
        expert_in, gate_w, up_w, down_w = operands
        gate_out = jnp.dot(expert_in, gate_w, preferred_element_type=jnp.float32)
        up_out = jnp.dot(expert_in, up_w, preferred_element_type=jnp.float32)
        active = (jax.nn.silu(gate_out) * up_out).astype(jnp.bfloat16)
        summed = jnp.zeros((expert_in.shape[0], D), jnp.float32)
        for group_index in range(N_TP):
            lower = group_index * hidden_width
            partial_value = jnp.dot(active[:, lower:lower + hidden_width], down_w[lower:lower + hidden_width], preferred_element_type=jnp.float32)
            summed = summed + lax.optimization_barrier(partial_value.astype(jnp.bfloat16)).astype(jnp.float32)
        return summed.astype(jnp.bfloat16)
    results = lax.map(run_expert, (stacked, gate_proj, up_proj, down_proj)).reshape(EXPERTS * blocks * CAP, D)
    first_weight = jax.nn.sigmoid(expert_score[:, 0] - expert_score[:, 1])
    combined = first_weight[:, None] * results[places[:, 0]].astype(jnp.float32) + (1.0 - first_weight)[:, None] * results[places[:, 1]].astype(jnp.float32)
    return (mixed_rows, combined.astype(jnp.bfloat16))
```

```python
import math

import jax
import jax.numpy as jnp
from jax import lax
from jax.sharding import Mesh
from jax.sharding import PartitionSpec as P

GRID_W = 64
EP = ("z", "core")
GRP_EP = ("grp", "z", "core")
GRP_EP_TP = ("grp", "z", "core", "tp")
EPS = 1e-06
THETA = 10000.0


def shifted(x, axis, distance):
    size = lax.axis_size(axis)
    return lax.ppermute(x, axis, [(i, (i + distance) % size) for i in range(size)])


def ring_step(x):
    size = lax.axis_size("z")
    pairs = []
    for i in range(size):
        pairs.append((2 * i, 2 * ((i + 1) % size)))
        pairs.append((2 * i + 1, 2 * ((i - 1) % size) + 1))
    return lax.ppermute(x, EP, pairs)


def head_norm(vectors, gain):
    return vectors * lax.rsqrt(jnp.mean(vectors * vectors, axis=-1, keepdims=True) + EPS) * gain


def rotate_grid(vectors, token_positions):
    length, heads, head_dim = vectors.shape
    quarter = head_dim // 4
    freqs = 1.0 / THETA ** (jnp.arange(quarter, dtype=jnp.float32) * 4.0 / head_dim)
    grid_row = (token_positions // GRID_W).astype(jnp.float32)
    grid_col = (token_positions % GRID_W).astype(jnp.float32)
    angles = jnp.stack([grid_row[:, None] * freqs, grid_col[:, None] * freqs], axis=1)
    cosine = jnp.cos(angles)[:, None]
    sine = jnp.sin(angles)[:, None]
    halves = vectors.reshape(length, heads, 2, 2, quarter)
    first = halves[..., 0, :]
    second = halves[..., 1, :]
    turned = jnp.stack([first * cosine - second * sine, second * cosine + first * sine], axis=-2)
    return turned.reshape(length, heads, head_dim)


def prepare_inputs(raw_rows, gain, heads, token_positions):
    length = raw_rows.shape[0]
    head_dim = gain.shape[0]
    vectors = raw_rows.astype(jnp.float32).reshape(length, heads, head_dim)
    return rotate_grid(head_norm(vectors, gain), token_positions).astype(jnp.bfloat16)


def gathered_keys_values(block):
    rows = block.shape[0]
    both = jnp.concatenate([block, shifted(block, "core", 1)], axis=0)
    steps = lax.axis_size("z") // 2
    arrived = []
    moving = both
    for step in range(steps):
        moving = ring_step(moving if step < steps - 1 else moving[:rows])
        arrived.append(moving)
    ours = jnp.concatenate(arrived, axis=0)
    return both, ours, shifted(ours, "core", 1)


def attention(query_matrix, keys_values, head_dim, score_scale):
    heads, length, _ = query_matrix.shape
    queries = query_matrix.reshape(heads * length, head_dim)
    rows = keys_values.shape[0]
    step_rows = math.gcd(rows, 1024)
    run_max = jnp.full((heads * length,), -1e30, jnp.float32)
    run_sum = jnp.zeros((heads * length,), jnp.float32)
    run_acc = jnp.zeros((heads * length, head_dim), jnp.float32)

    def one_block(index, running):
        run_max, run_sum, run_acc = running
        block = lax.dynamic_slice_in_dim(keys_values, index * step_rows, step_rows, 0)
        keys = block[:, :head_dim]
        values = block[:, head_dim:]
        scores = (
            lax.dot_general(
                queries, keys, (((1,), (1,)), ((), ())), preferred_element_type=jnp.float32
            )
            * score_scale
        )
        new_max = jnp.maximum(run_max, jnp.max(scores, axis=-1))
        factor = jnp.exp(run_max - new_max)
        weights = jnp.exp(scores - new_max[:, None])
        run_sum = run_sum * factor + jnp.sum(weights, axis=-1)
        update = jnp.dot(weights.astype(jnp.bfloat16), values, preferred_element_type=jnp.float32)
        return (new_max, run_sum, run_acc * factor[:, None] + update)

    run_max, run_sum, run_acc = lax.fori_loop(
        0, rows // step_rows, one_block, (run_max, run_sum, run_acc)
    )
    return (run_acc / run_sum[:, None]).astype(jnp.bfloat16).reshape(heads, length, head_dim)


def summed_over_tp(blocks):
    total = blocks[0].astype(jnp.float32)
    for distance in range(1, len(blocks)):
        total = total + shifted(blocks[distance], "tp", -distance).astype(jnp.float32)
    return total.astype(jnp.bfloat16)


def mixer_half(query_rows, projected_keys, projected_values, query_gain, key_norm_gain, out_proj):
    length = query_rows.shape[0]
    head_dim = query_gain.shape[0]
    q_heads = query_rows.shape[1] // head_dim
    tp = lax.axis_size("tp")
    token_positions = lax.axis_index(EP) * length + jnp.arange(length, dtype=jnp.int32)
    keys_turned = prepare_inputs(projected_keys, key_norm_gain, 1, token_positions).reshape(
        length, head_dim
    )
    block = jnp.concatenate([keys_turned, projected_values], axis=1)
    keys_values = jnp.concatenate(gathered_keys_values(block), axis=0)
    query_matrix = prepare_inputs(query_rows, query_gain, q_heads, token_positions).transpose(
        1, 0, 2
    )
    heads_out = attention(query_matrix, keys_values, head_dim, head_dim ** (-0.5))
    heads_out = heads_out.transpose(1, 0, 2).reshape(length, q_heads * head_dim)
    partial = jnp.dot(heads_out, out_proj, preferred_element_type=jnp.float32).astype(jnp.bfloat16)
    share = length // tp
    me = lax.axis_index("tp")
    blocks = [
        lax.dynamic_slice_in_dim(partial, lax.rem(me - d + tp, tp) * share, share, 0)
        for d in range(tp)
    ]
    return summed_over_tp(blocks)


def places_of(expert_ids, experts_all, capacity, source):
    chips = lax.axis_size("z")
    tokens = expert_ids.shape[0]
    named = expert_ids[:, :, None] == jnp.arange(experts_all, dtype=jnp.int32)
    either = jnp.any(named, axis=1).astype(jnp.bfloat16)
    order = jnp.arange(tokens, dtype=jnp.int32)
    earlier = (order[None, :] < order[:, None]).astype(jnp.bfloat16)
    before = jnp.dot(earlier, either, preferred_element_type=jnp.float32)
    slots = jnp.sum(jnp.where(named, before[:, None, :], 0.0), axis=-1).astype(jnp.int32)
    distance = lax.rem(expert_ids // 2 - lax.axis_index("z") + chips, chips)
    places = (distance * 2 + source) * capacity + slots
    return jnp.where(expert_ids % 2 == lax.axis_index("core"), places, -1)


def chunks_of_distances(chips):
    far = chips // 2
    order = [0]
    for distance in range(1, far):
        order += [distance, chips - distance]
    order.append(far)
    quarter = chips // 4
    near, second, third, last = (order[i * quarter : (i + 1) * quarter] for i in range(4))
    return [second, last, third, near]


def expert_half(mix_tokens, norm_gain, expert_ids, expert_score, gate_proj, up_proj, down_proj):
    length, model_dim = mix_tokens.shape
    top_count = expert_ids.shape[1]
    chips = lax.axis_size("z")
    tp = lax.axis_size("tp")
    experts_all = 2 * chips
    capacity = length * top_count * 3 // (2 * experts_all)
    tile = 2 * capacity
    gate, up, down = gate_proj[0], up_proj[0], down_proj[0]

    other_ids = shifted(expert_ids, "core", 1)
    other_tokens = shifted(mix_tokens, "core", 1)
    tokens = jnp.concatenate([mix_tokens, other_tokens], axis=0)
    values_b = tokens.astype(jnp.float32)
    normed = (
        values_b
        * lax.rsqrt(jnp.mean(values_b * values_b, axis=-1, keepdims=True) + EPS)
        * norm_gain
    ).astype(jnp.bfloat16)
    places = jnp.concatenate(
        [
            places_of(expert_ids, experts_all, capacity, 0),
            places_of(other_ids, experts_all, capacity, 1),
        ],
        axis=0,
    )
    at = jnp.arange(chips * tile, dtype=jnp.int32)
    chosen = [(places[:, k : k + 1] == at).astype(jnp.bfloat16) for k in range(top_count)]
    placed = sum(chosen[1:], chosen[0])
    outgoing = lax.dot_general(
        placed, normed, (((0,), (0,)), ((), ())), preferred_element_type=jnp.float32
    ).astype(jnp.bfloat16)

    returned = [None] * chips
    for group in chunks_of_distances(chips):
        own = jnp.concatenate(
            [
                outgoing[d * tile : (d + 1) * tile]
                if d == 0
                else shifted(outgoing[d * tile : (d + 1) * tile], "z", d)
                for d in group
            ],
            axis=0,
        )
        rows = own.shape[0]
        rows_in = jnp.concatenate([own] + [shifted(own, "tp", d) for d in range(1, tp)], axis=0)
        gate_out = jnp.dot(rows_in, gate, preferred_element_type=jnp.float32)
        up_out = jnp.dot(rows_in, up, preferred_element_type=jnp.float32)
        active = (jax.nn.silu(gate_out) * up_out).astype(jnp.bfloat16)
        partial = jnp.dot(active, down, preferred_element_type=jnp.float32).astype(jnp.bfloat16)
        summed = summed_over_tp([partial[d * rows : (d + 1) * rows] for d in range(tp)])
        for i, d in enumerate(group):
            piece = summed[i * tile : (i + 1) * tile]
            returned[d] = piece if d == 0 else shifted(piece, "z", -d)
    results = jnp.concatenate(returned, axis=0)
    picked = [
        jnp.dot(c, results, preferred_element_type=jnp.float32).astype(jnp.bfloat16) for c in chosen
    ]
    for_other = jnp.concatenate([p[length:] for p in picked], axis=0)
    from_other = shifted(for_other, "core", 1).reshape(top_count, length, model_dim)
    rows_of = [
        picked[k][:length].astype(jnp.float32) + from_other[k].astype(jnp.float32)
        for k in range(top_count)
    ]
    first_weight = jax.nn.sigmoid(expert_score[:, 0] - expert_score[:, 1])[:, None]
    return (first_weight * rows_of[0] + (1.0 - first_weight) * rows_of[1]).astype(jnp.bfloat16)


def local(
    query_rows,
    projected_keys,
    projected_values,
    query_gain,
    key_norm_gain,
    out_proj,
    mix_tokens,
    norm_gain,
    expert_ids,
    expert_score,
    gate_proj,
    up_proj,
    down_proj,
):
    mixed_rows = mixer_half(
        query_rows, projected_keys, projected_values, query_gain, key_norm_gain, out_proj
    )
    expert_out = expert_half(
        mix_tokens, norm_gain, expert_ids, expert_score, gate_proj, up_proj, down_proj
    )
    return (mixed_rows, expert_out)


def solution(mesh):
    split = Mesh(
        mesh.devices.reshape(mesh.shape["grp"], mesh.shape["ep"] // 2, 2, mesh.shape["tp"]),
        GRP_EP_TP,
    )
    return jax.shard_map(
        local,
        mesh=split,
        in_specs=(
            P(GRP_EP, "tp"),
            P(GRP_EP, "tp"),
            P(GRP_EP, "tp"),
            P(),
            P(),
            P("tp", None),
            P(GRP_EP_TP, None),
            P(),
            P(GRP_EP_TP, None),
            P(GRP_EP_TP, None),
            P(EP, None, "tp"),
            P(EP, None, "tp"),
            P(EP, "tp", None),
        ),
        out_specs=(P(GRP_EP_TP, None), P(GRP_EP_TP, None)),
        check_vma=False,
    )
```
